32 devices in a mesh: sp: 4 (over y, x), tp: 8 (over z, core).
Axes of the slice: x: 2, y: 2, z: 4, core: 2. Of those that a mesh axis runs over, the one named last changes fastest.
Arguments:
- tokens: bfloat16 [2048, 4096], P('sp', 'tp'), may hold values from -6 to 6
- pre_gain: float32 [2, 4096], replicated, may hold values from 0.1 to 1.9
- w_value: bfloat16 [2, 4096, 4096], P(None, 'sp', 'tp'), may hold values from -0.09375 to 0.09375
- w_gate: bfloat16 [2, 4096, 4096], P(None, 'sp', 'tp'), may hold values from -0.09375 to 0.09375
- conv_taps: float32 [2, 31, 4096], P(None, None, 'tp'), may hold values from -3.5 to 3.5
- conv_bias: float32 [2, 4096], P(None, 'tp'), may hold values from -3 to 3
- norm_gain: float32 [2, 4096], P(None, 'tp'), may hold values from 0.1 to 1.9
- norm_bias: float32 [2, 4096], P(None, 'tp'), may hold values from -3 to 3
- w_out: bfloat16 [2, 4096, 4096], P(None, 'sp', 'tp'), may hold values from -0.09375 to 0.09375
- post_gain: float32 [2, 4096], P(None, 'tp'), may hold values from 0.1 to 1.9
Outputs:
- stream: bfloat16 [2048, 4096], P('sp', 'tp')
The draws below stay inside these ranges and needn't reach their ends.
All inputs are finite; a program needn't handle non-finite values.
Results may differ from the reference program's by a relative error of at most 0.009.
Values may be sent and summed in bfloat16 or wider, within the bound.
A program may use at most 64 MiB of HBM per device.

```python
import math
import jax
import jax.numpy as jnp
from jax import lax

D = 4096
CH = 4096
TAPS = 31
LAYERS = 2
TOKENS = 2048


def draw_conv_taps(key, part):
    first_key, second_key, third_key = jax.random.split(key, 3)
    channel = jnp.arange(CH, dtype=jnp.float32)
    phase = jax.random.uniform(first_key, (LAYERS, 1, 1), jnp.float32, 0.0, 2.0 * math.pi)
    rough = jax.random.uniform(second_key, (LAYERS, 1, CH), jnp.float32, -0.35, 0.35)
    factor = jnp.exp(1.2 * jnp.sin(2.0 * math.pi * 3.0 * channel / CH + phase) + rough)
    base = jnp.clip(jax.random.normal(third_key, (LAYERS, TAPS, CH), jnp.float32), -4.0, 4.0)
    return base * factor / math.sqrt(TAPS)


def steps_of(own_key, shape, shards, smallest, high):
    def one(position, blocks):
        steps = jax.random.uniform(jax.random.fold_in(jax.random.fold_in(own_key, 6), position), (blocks,), jnp.float32, smallest / len(shards), high / len(shards))
        return jnp.repeat(jnp.exp(steps), shape[position] // blocks).reshape((-1,) + (1,) * (len(shape) - position - 1))

    level = one(*shards[0])
    for cut in shards[1:]:
        level = level * one(*cut)
    return level


def scatter_about(own_key, shape, width, limit, cuts=(), held_as=jnp.bfloat16):
    entries = width * jax.random.normal(own_key, shape, jnp.float32)
    if cuts:
        entries = entries * steps_of(own_key, shape, cuts, -0.22, 0.18)
    return jnp.clip(entries, -limit, limit).astype(held_as)


def setup_inputs(seed: int = 0) -> dict:
    keys = jax.random.split(jax.random.key(seed), 11)
    tokens = scatter_about(keys[0], (TOKENS, D), 1.0, 6.0, ((0, 4), (1, 8)))
    pre_gain = jnp.clip(1.0 + 0.18 * jax.random.normal(keys[1], (LAYERS, D), jnp.float32), 0.1, 1.9)
    w_value = scatter_about(keys[2], (LAYERS, D, CH), D ** -0.5, 0.09375, ((1, 4), (2, 8)))
    w_gate = scatter_about(keys[3], (LAYERS, D, CH), D ** -0.5, 0.09375, ((1, 4), (2, 8)))
    conv_taps = draw_conv_taps(jax.random.fold_in(keys[10], 71), 0)
    conv_bias = scatter_about(keys[5], (LAYERS, CH), 0.5, 3.0, ((1, 8),), jnp.float32)
    norm_gain = jnp.clip(1.0 + 0.18 * jax.random.normal(keys[6], (LAYERS, CH), jnp.float32), 0.1, 1.9)
    norm_bias = scatter_about(keys[7], (LAYERS, CH), 0.5, 3.0, ((1, 8),), jnp.float32)
    w_out = scatter_about(keys[8], (LAYERS, CH, D), CH ** -0.5, 0.09375, ((1, 4), (2, 8)))
    post_gain = jnp.clip(1.0 + 0.18 * jax.random.normal(keys[9], (LAYERS, D), jnp.float32), 0.1, 1.9)
    return dict(tokens=tokens, pre_gain=pre_gain, w_value=w_value, w_gate=w_gate, conv_taps=conv_taps, conv_bias=conv_bias, norm_gain=norm_gain, norm_bias=norm_bias, w_out=w_out, post_gain=post_gain)


def reference(tokens, pre_gain, w_value, w_gate, conv_taps, conv_bias, norm_gain, norm_bias, w_out, post_gain):
    stream = tokens
    for layer_index in range(LAYERS):
        full_rows = stream.astype(jnp.float32)
        scale_rows = lax.rsqrt(lax.optimization_barrier(jnp.mean(full_rows * full_rows, axis=-1, keepdims=True)) + 1e-06)
        normed = (full_rows * scale_rows * pre_gain[layer_index]).astype(jnp.bfloat16)
        value_proj = jnp.dot(normed, w_value[layer_index], preferred_element_type=jnp.float32)
        gate_proj = jnp.dot(normed, w_gate[layer_index], preferred_element_type=jnp.float32)
        glu_out = (value_proj * jax.nn.sigmoid(gate_proj)).astype(jnp.bfloat16)
        padded = jnp.concatenate([jnp.zeros((TAPS - 1, CH), jnp.bfloat16), glu_out], axis=0).astype(jnp.float32)
        filtered = jnp.zeros((TOKENS, CH), jnp.float32) + conv_bias[layer_index]
        for tap_index in range(TAPS):
            filtered = filtered + padded[tap_index:tap_index + TOKENS] * conv_taps[layer_index, tap_index]
        centre = lax.optimization_barrier(jnp.sum(filtered, axis=-1)) / CH
        spread = jnp.maximum(lax.optimization_barrier(jnp.sum(filtered * filtered, axis=-1)) / CH - centre * centre, 0.0)
        shaped = (filtered - centre[:, None]) * lax.rsqrt(spread + 1e-05)[:, None]
        mixed = jax.nn.silu(shaped * norm_gain[layer_index] + norm_bias[layer_index]).astype(jnp.bfloat16)
        branch_low = jnp.dot(mixed, w_out[layer_index], preferred_element_type=jnp.float32).astype(jnp.bfloat16)
        branch = lax.optimization_barrier(branch_low).astype(jnp.float32)
        total = lax.optimization_barrier(jnp.sum(branch * branch, axis=-1))
        rescale = lax.rsqrt(total / D + 1e-06)[:, None]
        stream = (stream.astype(jnp.float32) + branch * rescale * post_gain[layer_index]).astype(jnp.bfloat16)
    return stream
```

```python
import functools

import jax
import jax.numpy as jnp
from jax import lax
from jax.experimental import pallas as pl
from jax.experimental.pallas import tpu as pltpu
from jax.sharding import PartitionSpec as P

MESH = pl.DeviceIdType.MESH


def gather_kernel(chips, x_ref, out_ref, up_send, up_recv, down_send, down_recv, side_send, side_recv):
    me = lax.axis_index("tp")
    z = me // 2
    core = me - 2 * z
    partner = me + 1 - 2 * core
    width = x_ref.shape[1]
    has_up = z < chips - 1
    has_down = z > 0

    barrier = pltpu.get_barrier_semaphore()
    pl.semaphore_signal(barrier, inc=1, device_id={"tp": partner}, device_id_type=MESH)

    @pl.when(has_up)
    def _():
        pl.semaphore_signal(barrier, inc=1, device_id={"tp": me + 2}, device_id_type=MESH)

    @pl.when(has_down)
    def _():
        pl.semaphore_signal(barrier, inc=1, device_id={"tp": me - 2}, device_id_type=MESH)

    pl.semaphore_wait(barrier, 1 + has_up.astype(jnp.int32) + has_down.astype(jnp.int32))

    def place(chip):
        return out_ref.at[:, pl.ds(pl.multiple_of((2 * chip + core) * width, width), width)]

    def send(own, chip, sends, recvs, index, target):
        return pltpu.make_async_remote_copy(
            src_ref=x_ref if own else place(chip),
            dst_ref=place(chip),
            send_sem=sends.at[index],
            recv_sem=recvs.at[index],
            device_id={"tp": target},
            device_id_type=MESH,
        )

    def up(step):
        return send(step == 0, z - step, up_send, up_recv, step, me + 2)

    def down(step):
        return send(step == 0, z + step, down_send, down_recv, step, me - 2)

    def side(chip, index):
        return send(index == 0, chip, side_send, side_recv, index, partner)

    @pl.when(has_up)
    def _():
        up(0).start()

    @pl.when(has_down)
    def _():
        down(0).start()

    side(z, 0).start()
    out_ref[:, pl.ds(pl.multiple_of(me * width, width), width)] = x_ref[...]

    for step in range(chips - 1):

        @pl.when(z - 1 - step >= 0)
        def _():
            up(step).wait_recv()
            if step + 1 < chips - 1:

                @pl.when(has_up)
                def _():
                    up(step + 1).start()

            side(z - 1 - step, 1 + step).start()

        @pl.when(z + 1 + step < chips)
        def _():
            down(step).wait_recv()
            if step + 1 < chips - 1:

                @pl.when(has_down)
                def _():
                    down(step + 1).start()

            side(z + 1 + step, chips + step).start()

    side(z, 0).wait()
    for step in range(chips - 1):

        @pl.when(z - 1 - step >= 0)
        def _():
            side(z - 1 - step, 1 + step).wait()

        @pl.when(z + 1 + step < chips)
        def _():
            side(z + 1 + step, chips + step).wait()

        @pl.when(has_up & (z - step >= 0))
        def _():
            up(step).wait_send()

        @pl.when(has_down & (z + step < chips))
        def _():
            down(step).wait_send()


def gather_over_tp(block, collective_id):
    count = lax.axis_size("tp")
    chips = count // 2
    rows, width = block.shape
    return pl.pallas_call(
        functools.partial(gather_kernel, chips),
        out_shape=jax.ShapeDtypeStruct((rows, width * count), block.dtype),
        in_specs=[pl.BlockSpec(memory_space=pltpu.VMEM)],
        out_specs=pl.BlockSpec(memory_space=pltpu.VMEM),
        scratch_shapes=[pltpu.SemaphoreType.DMA((chips - 1,))] * 4
        + [pltpu.SemaphoreType.DMA((2 * chips - 1,))] * 2,
        compiler_params=pltpu.CompilerParams(
            collective_id=collective_id, has_side_effects=True, vmem_limit_bytes=16 * 2**20
        ),
        cost_estimate=pl.CostEstimate(
            flops=COST_FLOPS, bytes_accessed=rows * width * count * 2, transcendentals=0
        ),
        name="gather_tp",
    )(block)


COST_FLOPS = 20 * 10**9


def sum_kernel(count, x_ref, out_ref, slots, sends, recvs):
    me = lax.axis_index("tp")
    barrier = pltpu.get_barrier_semaphore()
    for step in range(1, count):
        pl.semaphore_signal(
            barrier, inc=1, device_id={"tp": lax.rem(me + step, count)}, device_id_type=MESH
        )
    pl.semaphore_wait(barrier, count - 1)
    copies = [
        pltpu.make_async_remote_copy(
            src_ref=x_ref,
            dst_ref=slots.at[step - 1],
            send_sem=sends.at[step - 1],
            recv_sem=recvs.at[step - 1],
            device_id={"tp": lax.rem(me + step, count)},
            device_id_type=MESH,
        )
        for step in range(1, count)
    ]
    for copy in copies:
        copy.start()
    total = x_ref[...]
    for step in range(1, count):
        copies[step - 1].wait_recv()
        total = total + slots[step - 1]
    out_ref[...] = total
    for copy in copies:
        copy.wait_send()


def sum_over_tp(parts, collective_id):
    count = lax.axis_size("tp")
    flat = jnp.stack(parts).reshape(-1, 128)
    total = pl.pallas_call(
        functools.partial(sum_kernel, count),
        out_shape=jax.ShapeDtypeStruct(flat.shape, flat.dtype),
        in_specs=[pl.BlockSpec(memory_space=pltpu.VMEM)],
        out_specs=pl.BlockSpec(memory_space=pltpu.VMEM),
        scratch_shapes=[
            pltpu.VMEM((count - 1,) + flat.shape, flat.dtype),
            pltpu.SemaphoreType.DMA((count - 1,)),
            pltpu.SemaphoreType.DMA((count - 1,)),
        ],
        compiler_params=pltpu.CompilerParams(
            collective_id=collective_id, has_side_effects=True, vmem_limit_bytes=4 * 2**20
        ),
        cost_estimate=pl.CostEstimate(
            flops=COST_FLOPS // 8, bytes_accessed=flat.size * 8, transcendentals=0
        ),
        name="sum_tp",
    )(flat)
    return total.reshape(len(parts), -1)


def passed_along(value, axis, steps):
    count = lax.axis_size(axis)
    leading, last = (max(0, -steps), min(count, count - steps))
    return lax.ppermute(value, axis, [(source, source + steps) for source in range(leading, last)])


def shards(
    tokens, pre_gain, w_value, w_gate, conv_taps, conv_bias, norm_gain, norm_bias, w_out, post_gain
):
    layer_count = w_value.shape[0]
    tap_count = conv_taps.shape[1]
    channel_count = conv_taps.shape[2] * lax.axis_size("tp")
    model_width = tokens.shape[1] * lax.axis_size("tp")
    local_rows = tokens.shape[0]
    whole = []
    for layer_index in range(layer_count):
        per_layer = []
        for block in (w_value, w_gate, w_out):
            per_layer.append(lax.all_gather(block[layer_index], "sp", axis=0, tiled=True))
        whole.append(per_layer)
    stream = tokens
    for layer_index in range(layer_count):
        value_block, gate_block, out_block = whole[layer_index]
        gathered = gather_over_tp(stream, 4 * layer_index)
        full_rows = gathered.astype(jnp.float32)
        scale_rows = lax.rsqrt(jnp.mean(full_rows * full_rows, axis=-1, keepdims=True) + 1e-06)
        normed = (full_rows * scale_rows * pre_gain[layer_index]).astype(jnp.bfloat16)
        value_proj = jnp.dot(normed, value_block, preferred_element_type=jnp.float32)
        gate_proj = jnp.dot(normed, gate_block, preferred_element_type=jnp.float32)
        glu_out = (value_proj * jax.nn.sigmoid(gate_proj)).astype(jnp.bfloat16)
        earlier = passed_along(glu_out[local_rows - (tap_count - 1) :], "sp", 1)
        padded = jnp.concatenate([earlier, glu_out], axis=0).astype(jnp.float32)
        filtered = jnp.zeros(glu_out.shape, jnp.float32) + conv_bias[layer_index]
        for tap_index in range(tap_count):
            filtered = (
                filtered
                + padded[tap_index : tap_index + local_rows] * conv_taps[layer_index, tap_index]
            )
        channel_sum, channel_square = sum_over_tp(
            (jnp.sum(filtered, axis=-1), jnp.sum(filtered * filtered, axis=-1)), 4 * layer_index + 1
        )
        centre = channel_sum / channel_count
        spread = jnp.maximum(channel_square / channel_count - centre * centre, 0.0)
        shaped = (filtered - centre[:, None]) * lax.rsqrt(spread + 1e-05)[:, None]
        mixed = jax.nn.silu(shaped * norm_gain[layer_index] + norm_bias[layer_index]).astype(
            jnp.bfloat16
        )
        whole_mixed = gather_over_tp(mixed, 4 * layer_index + 2)
        branch_low = jnp.dot(whole_mixed, out_block, preferred_element_type=jnp.float32).astype(
            jnp.bfloat16
        )
        branch = lax.optimization_barrier(branch_low).astype(jnp.float32)
        (total,) = sum_over_tp((jnp.sum(branch * branch, axis=-1),), 4 * layer_index + 3)
        rescale = lax.rsqrt(total / model_width + 1e-06)[:, None]
        stream = (stream.astype(jnp.float32) + branch * rescale * post_gain[layer_index]).astype(
            jnp.bfloat16
        )
    return stream


def solution(mesh):
    in_specs = (
        P("sp", "tp"),
        P(),
        P(None, "sp", "tp"),
        P(None, "sp", "tp"),
        P(None, None, "tp"),
        P(None, "tp"),
        P(None, "tp"),
        P(None, "tp"),
        P(None, "sp", "tp"),
        P(None, "tp"),
    )
    out_specs = P("sp", "tp")
    return jax.shard_map(shards, mesh=mesh, in_specs=in_specs, out_specs=out_specs, check_vma=False)
```

```python
import functools

import jax
import jax.numpy as jnp
from jax import lax
from jax.experimental import pallas as pl
from jax.experimental.pallas import tpu as pltpu
from jax.sharding import PartitionSpec as P

MESH = pl.DeviceIdType.MESH


def gray_of(position, count):
    bits = [(position // 2**k) % 2 for k in range(count.bit_length())]
    return sum(((bits[k] + bits[k + 1]) % 2) * 2**k for k in range(count.bit_length() - 1))


def position_of(index, count):
    bits = [(index // 2**k) % 2 for k in range(count.bit_length() - 1)]
    return sum((sum(bits[k:]) % 2) * 2**k for k in range(count.bit_length() - 1))


def gather_kernel(chips, ring, layer, *refs):
    if ring:
        x_ref, w_ref, out_ref, rows_ref = refs[:4]
        next_send, next_recv, last_send, last_recv, own_sem = refs[10:]
        refs = refs[4:10]
    else:
        x_ref, out_ref = refs[:2]
        refs = refs[2:]
    up_send, up_recv, down_send, down_recv, side_send, side_recv = refs
    me = lax.axis_index("tp")
    z = me // 2
    core = me - 2 * z
    partner = me + 1 - 2 * core
    width = x_ref.shape[1]
    has_up = z < chips - 1
    has_down = z > 0

    barrier = pltpu.get_barrier_semaphore()
    pl.semaphore_signal(barrier, inc=1, device_id={"tp": partner}, device_id_type=MESH)

    @pl.when(has_up)
    def _():
        pl.semaphore_signal(barrier, inc=1, device_id={"tp": me + 2}, device_id_type=MESH)

    @pl.when(has_down)
    def _():
        pl.semaphore_signal(barrier, inc=1, device_id={"tp": me - 2}, device_id_type=MESH)

    if ring:
        at = position_of(lax.axis_index("sp"), ring)
        ahead = gray_of((at + 1) % ring, ring)
        behind = gray_of((at + ring - 1) % ring, ring)
        pl.semaphore_signal(barrier, inc=1, device_id={"sp": ahead}, device_id_type=MESH)
        pl.semaphore_signal(barrier, inc=1, device_id={"sp": behind}, device_id_type=MESH)

    pl.semaphore_wait(barrier, (3 if ring else 1) + has_up.astype(jnp.int32) + has_down.astype(jnp.int32))

    def place(chip):
        return out_ref.at[:, pl.ds(pl.multiple_of((2 * chip + core) * width, width), width)]

    def send(own, chip, sends, recvs, index, target):
        return pltpu.make_async_remote_copy(
            src_ref=x_ref if own else place(chip),
            dst_ref=place(chip),
            send_sem=sends.at[index],
            recv_sem=recvs.at[index],
            device_id={"tp": target},
            device_id_type=MESH,
        )

    def up(step):
        return send(step == 0, z - step, up_send, up_recv, step, me + 2)

    def down(step):
        return send(step == 0, z + step, down_send, down_recv, step, me - 2)

    def side(chip, index):
        return send(index == 0, chip, side_send, side_recv, index, partner)

    if ring:
        depth = w_ref.shape[1]

        def held(owner, first, size):
            start = pl.multiple_of(owner * depth + first, size)
            return rows_ref.at[pl.ds(start, size), :]

        def ring_send(step, sign, sends, recvs, target):
            owner = gray_of((at + ring - sign * step) % ring, ring)
            last = step == ring // 2 - 1
            size = depth // 2 if last else depth
            first = depth // 2 if last and sign < 0 else 0
            place_there = held(owner, first, size)
            own = w_ref.at[layer, pl.ds(first, size), :]
            return pltpu.make_async_remote_copy(
                src_ref=own if step == 0 else place_there,
                dst_ref=place_there,
                send_sem=sends.at[step],
                recv_sem=recvs.at[step],
                device_id={"sp": target},
                device_id_type=MESH,
            )

        def forward(step):
            return ring_send(step, 1, next_send, next_recv, ahead)

        def backward(step):
            return ring_send(step, -1, last_send, last_recv, behind)

        forward(0).start()
        backward(0).start()
        own_copy = pltpu.make_async_copy(
            w_ref.at[layer], held(lax.axis_index("sp"), 0, depth), own_sem
        )
        own_copy.start()

    @pl.when(has_up)
    def _():
        up(0).start()

    @pl.when(has_down)
    def _():
        down(0).start()

    side(z, 0).start()
    out_ref[:, pl.ds(pl.multiple_of(me * width, width), width)] = x_ref[...]

    def ring_turn(step):
        forward(step).wait_recv()
        forward(step + 1).start()
        backward(step).wait_recv()
        backward(step + 1).start()

    for step in range(chips - 1):

        @pl.when(z - 1 - step >= 0)
        def _():
            up(step).wait_recv()
            if step + 1 < chips - 1:

                @pl.when(has_up)
                def _():
                    up(step + 1).start()

            side(z - 1 - step, 1 + step).start()

        @pl.when(z + 1 + step < chips)
        def _():
            down(step).wait_recv()
            if step + 1 < chips - 1:

                @pl.when(has_down)
                def _():
                    down(step + 1).start()

            side(z + 1 + step, chips + step).start()

        if ring and 1 <= step and step < ring // 2:
            ring_turn(step - 1)

    if ring:
        for step in range(chips - 2, ring // 2 - 1):
            ring_turn(step)
        forward(ring // 2 - 1).wait_recv()
        backward(ring // 2 - 1).wait_recv()
        for step in range(ring // 2):
            forward(step).wait_send()
            backward(step).wait_send()
        own_copy.wait()
    side(z, 0).wait()
    for step in range(chips - 1):

        @pl.when(z - 1 - step >= 0)
        def _():
            side(z - 1 - step, 1 + step).wait()

        @pl.when(z + 1 + step < chips)
        def _():
            side(z + 1 + step, chips + step).wait()

        @pl.when(has_up & (z - step >= 0))
        def _():
            up(step).wait_send()

        @pl.when(has_down & (z + step < chips))
        def _():
            down(step).wait_send()


def gather_over_tp(block, collective_id, weights=None, layer=0):
    count = lax.axis_size("tp")
    chips = count // 2
    rows, width = block.shape
    ring = 0 if weights is None else lax.axis_size("sp")
    operands = [block]
    in_specs = [pl.BlockSpec(memory_space=pltpu.VMEM)]
    out_shape = [jax.ShapeDtypeStruct((rows, width * count), block.dtype)]
    scratch = [pltpu.SemaphoreType.DMA((chips - 1,))] * 4
    scratch += [pltpu.SemaphoreType.DMA((2 * chips - 1,))] * 2
    if ring:
        operands.append(weights)
        in_specs.append(pl.BlockSpec(memory_space=pl.ANY))
        out_shape.append(
            jax.ShapeDtypeStruct((weights.shape[1] * ring, weights.shape[2]), weights.dtype)
        )
        scratch += [pltpu.SemaphoreType.DMA((ring // 2,))] * 4
        scratch += [pltpu.SemaphoreType.DMA]
    results = pl.pallas_call(
        functools.partial(gather_kernel, chips, ring, layer),
        out_shape=out_shape,
        in_specs=in_specs,
        out_specs=[pl.BlockSpec(memory_space=pltpu.VMEM)] * len(out_shape),
        scratch_shapes=scratch,
        compiler_params=pltpu.CompilerParams(
            collective_id=collective_id,
            has_side_effects=True,
            vmem_limit_bytes=(48 if ring else 16) * 2**20,
        ),
        cost_estimate=pl.CostEstimate(
            flops=COST_FLOPS, bytes_accessed=rows * width * count * 2, transcendentals=0
        ),
        name="gather_tp",
    )(*operands)
    return results if ring else results[0]


COST_FLOPS = 20 * 10**9


def sum_kernel(count, x_ref, out_ref, slots, sends, recvs):
    me = lax.axis_index("tp")
    barrier = pltpu.get_barrier_semaphore()
    for step in range(1, count):
        pl.semaphore_signal(
            barrier, inc=1, device_id={"tp": lax.rem(me + step, count)}, device_id_type=MESH
        )
    pl.semaphore_wait(barrier, count - 1)
    copies = [
        pltpu.make_async_remote_copy(
            src_ref=x_ref,
            dst_ref=slots.at[step - 1],
            send_sem=sends.at[step - 1],
            recv_sem=recvs.at[step - 1],
            device_id={"tp": lax.rem(me + step, count)},
            device_id_type=MESH,
        )
        for step in range(1, count)
    ]
    for copy in copies:
        copy.start()
    total = x_ref[...]
    for step in range(1, count):
        copies[step - 1].wait_recv()
        total = total + slots[step - 1]
    out_ref[...] = total
    for copy in copies:
        copy.wait_send()


def sum_over_tp(parts, collective_id):
    count = lax.axis_size("tp")
    flat = jnp.stack(parts).reshape(-1, 128)
    total = pl.pallas_call(
        functools.partial(sum_kernel, count),
        out_shape=jax.ShapeDtypeStruct(flat.shape, flat.dtype),
        in_specs=[pl.BlockSpec(memory_space=pltpu.VMEM)],
        out_specs=pl.BlockSpec(memory_space=pltpu.VMEM),
        scratch_shapes=[
            pltpu.VMEM((count - 1,) + flat.shape, flat.dtype),
            pltpu.SemaphoreType.DMA((count - 1,)),
            pltpu.SemaphoreType.DMA((count - 1,)),
        ],
        compiler_params=pltpu.CompilerParams(
            collective_id=collective_id, has_side_effects=True, vmem_limit_bytes=4 * 2**20
        ),
        cost_estimate=pl.CostEstimate(
            flops=COST_FLOPS // 8, bytes_accessed=flat.size * 8, transcendentals=0
        ),
        name="sum_tp",
    )(flat)
    return total.reshape(len(parts), -1)


def passed_along(value, axis, steps):
    count = lax.axis_size(axis)
    leading, last = (max(0, -steps), min(count, count - steps))
    return lax.ppermute(value, axis, [(source, source + steps) for source in range(leading, last)])


def shards(
    tokens, pre_gain, w_value, w_gate, conv_taps, conv_bias, norm_gain, norm_bias, w_out, post_gain
):
    layer_count = w_value.shape[0]
    tap_count = conv_taps.shape[1]
    channel_count = conv_taps.shape[2] * lax.axis_size("tp")
    model_width = tokens.shape[1] * lax.axis_size("tp")
    local_rows = tokens.shape[0]
    whole = []
    for layer_index in range(layer_count):
        per_layer = []
        for block in (w_gate, w_out):
            per_layer.append(lax.all_gather(block[layer_index], "sp", axis=0, tiled=True))
        whole.append(per_layer)
    stream = tokens
    for layer_index in range(layer_count):
        gate_block, out_block = whole[layer_index]
        gathered, value_block = gather_over_tp(stream, 4 * layer_index, w_value, layer_index)
        full_rows = gathered.astype(jnp.float32)
        scale_rows = lax.rsqrt(jnp.mean(full_rows * full_rows, axis=-1, keepdims=True) + 1e-06)
        normed = (full_rows * scale_rows * pre_gain[layer_index]).astype(jnp.bfloat16)
        value_proj = jnp.dot(normed, value_block, preferred_element_type=jnp.float32)
        gate_proj = jnp.dot(normed, gate_block, preferred_element_type=jnp.float32)
        glu_out = (value_proj * jax.nn.sigmoid(gate_proj)).astype(jnp.bfloat16)
        earlier = passed_along(glu_out[local_rows - (tap_count - 1) :], "sp", 1)
        padded = jnp.concatenate([earlier, glu_out], axis=0).astype(jnp.float32)
        filtered = jnp.zeros(glu_out.shape, jnp.float32) + conv_bias[layer_index]
        for tap_index in range(tap_count):
            filtered = (
                filtered
                + padded[tap_index : tap_index + local_rows] * conv_taps[layer_index, tap_index]
            )
        channel_sum, channel_square = sum_over_tp(
            (jnp.sum(filtered, axis=-1), jnp.sum(filtered * filtered, axis=-1)), 4 * layer_index + 1
        )
        centre = channel_sum / channel_count
        spread = jnp.maximum(channel_square / channel_count - centre * centre, 0.0)
        shaped = (filtered - centre[:, None]) * lax.rsqrt(spread + 1e-05)[:, None]
        mixed = jax.nn.silu(shaped * norm_gain[layer_index] + norm_bias[layer_index]).astype(
            jnp.bfloat16
        )
        whole_mixed = gather_over_tp(mixed, 4 * layer_index + 2)
        branch_low = jnp.dot(whole_mixed, out_block, preferred_element_type=jnp.float32).astype(
            jnp.bfloat16
        )
        branch = lax.optimization_barrier(branch_low).astype(jnp.float32)
        (total,) = sum_over_tp((jnp.sum(branch * branch, axis=-1),), 4 * layer_index + 3)
        rescale = lax.rsqrt(total / model_width + 1e-06)[:, None]
        stream = (stream.astype(jnp.float32) + branch * rescale * post_gain[layer_index]).astype(
            jnp.bfloat16
        )
    return stream


def solution(mesh):
    in_specs = (
        P("sp", "tp"),
        P(),
        P(None, "sp", "tp"),
        P(None, "sp", "tp"),
        P(None, None, "tp"),
        P(None, "tp"),
        P(None, "tp"),
        P(None, "tp"),
        P(None, "sp", "tp"),
        P(None, "tp"),
    )
    out_specs = P("sp", "tp")
    return jax.shard_map(shards, mesh=mesh, in_specs=in_specs, out_specs=out_specs, check_vma=False)
```

```python
import functools

import jax
import jax.numpy as jnp
from jax import lax
from jax.experimental import pallas as pl
from jax.experimental.pallas import tpu as pltpu
from jax.sharding import PartitionSpec as P

MESH = pl.DeviceIdType.MESH


def gray_of(position, count):
    bits = [(position // 2**k) % 2 for k in range(count.bit_length())]
    return sum(((bits[k] + bits[k + 1]) % 2) * 2**k for k in range(count.bit_length() - 1))


def position_of(index, count):
    bits = [(index // 2**k) % 2 for k in range(count.bit_length() - 1)]
    return sum((sum(bits[k:]) % 2) * 2**k for k in range(count.bit_length() - 1))


def gather_kernel(chips, ring, layer, *refs):
    if ring:
        x_ref, w_ref, out_ref, rows_ref = refs[:4]
        next_send, next_recv, last_send, last_recv, own_sem = refs[10:]
        refs = refs[4:10]
    else:
        x_ref, out_ref = refs[:2]
        refs = refs[2:]
    up_send, up_recv, down_send, down_recv, side_send, side_recv = refs
    me = lax.axis_index("tp")
    z = me // 2
    core = me - 2 * z
    partner = me + 1 - 2 * core
    width = x_ref.shape[1]
    has_up = z < chips - 1
    has_down = z > 0

    barrier = pltpu.get_barrier_semaphore()
    pl.semaphore_signal(barrier, inc=1, device_id={"tp": partner}, device_id_type=MESH)

    @pl.when(has_up)
    def _():
        pl.semaphore_signal(barrier, inc=1, device_id={"tp": me + 2}, device_id_type=MESH)

    @pl.when(has_down)
    def _():
        pl.semaphore_signal(barrier, inc=1, device_id={"tp": me - 2}, device_id_type=MESH)

    if ring:
        at = position_of(lax.axis_index("sp"), ring)
        ahead = gray_of((at + 1) % ring, ring)
        behind = gray_of((at + ring - 1) % ring, ring)
        pl.semaphore_signal(barrier, inc=1, device_id={"sp": ahead}, device_id_type=MESH)
        pl.semaphore_signal(barrier, inc=1, device_id={"sp": behind}, device_id_type=MESH)

    pl.semaphore_wait(barrier, (3 if ring else 1) + has_up.astype(jnp.int32) + has_down.astype(jnp.int32))

    def place(chip):
        return out_ref.at[:, pl.ds(pl.multiple_of((2 * chip + core) * width, width), width)]

    def send(own, chip, sends, recvs, index, target):
        return pltpu.make_async_remote_copy(
            src_ref=x_ref if own else place(chip),
            dst_ref=place(chip),
            send_sem=sends.at[index],
            recv_sem=recvs.at[index],
            device_id={"tp": target},
            device_id_type=MESH,
        )

    def up(step):
        return send(step == 0, z - step, up_send, up_recv, step, me + 2)

    def down(step):
        return send(step == 0, z + step, down_send, down_recv, step, me - 2)

    def side(chip, index):
        return send(index == 0, chip, side_send, side_recv, index, partner)

    if ring:
        depth = w_ref.shape[1]

        def held(owner, first, size):
            start = pl.multiple_of(owner * depth + first, size)
            return rows_ref.at[pl.ds(start, size), :]

        def ring_send(step, sign, sends, recvs, target):
            owner = gray_of((at + ring - sign * step) % ring, ring)
            last = step == ring // 2 - 1
            size = depth // 2 if last else depth
            first = depth // 2 if last and sign < 0 else 0
            place_there = held(owner, first, size)
            own = w_ref.at[layer, pl.ds(first, size), :]
            return pltpu.make_async_remote_copy(
                src_ref=own if step == 0 else place_there,
                dst_ref=place_there,
                send_sem=sends.at[step],
                recv_sem=recvs.at[step],
                device_id={"sp": target},
                device_id_type=MESH,
            )

        def forward(step):
            return ring_send(step, 1, next_send, next_recv, ahead)

        def backward(step):
            return ring_send(step, -1, last_send, last_recv, behind)

        forward(0).start()
        backward(0).start()
        own_copy = pltpu.make_async_copy(
            w_ref.at[layer], held(lax.axis_index("sp"), 0, depth), own_sem
        )
        own_copy.start()

    @pl.when(has_up)
    def _():
        up(0).start()

    @pl.when(has_down)
    def _():
        down(0).start()

    side(z, 0).start()
    out_ref[:, pl.ds(pl.multiple_of(me * width, width), width)] = x_ref[...]

    def ring_turn(step):
        forward(step).wait_recv()
        forward(step + 1).start()
        backward(step).wait_recv()
        backward(step + 1).start()

    for step in range(chips - 1):

        @pl.when(z - 1 - step >= 0)
        def _():
            up(step).wait_recv()
            if step + 1 < chips - 1:

                @pl.when(has_up)
                def _():
                    up(step + 1).start()

            side(z - 1 - step, 1 + step).start()

        @pl.when(z + 1 + step < chips)
        def _():
            down(step).wait_recv()
            if step + 1 < chips - 1:

                @pl.when(has_down)
                def _():
                    down(step + 1).start()

            side(z + 1 + step, chips + step).start()

        if ring and 1 <= step and step < ring // 2:
            ring_turn(step - 1)

    if ring:
        for step in range(chips - 2, ring // 2 - 1):
            ring_turn(step)
        forward(ring // 2 - 1).wait_recv()
        backward(ring // 2 - 1).wait_recv()
        for step in range(ring // 2):
            forward(step).wait_send()
            backward(step).wait_send()
        own_copy.wait()
    side(z, 0).wait()
    for step in range(chips - 1):

        @pl.when(z - 1 - step >= 0)
        def _():
            side(z - 1 - step, 1 + step).wait()

        @pl.when(z + 1 + step < chips)
        def _():
            side(z + 1 + step, chips + step).wait()

        @pl.when(has_up & (z - step >= 0))
        def _():
            up(step).wait_send()

        @pl.when(has_down & (z + step < chips))
        def _():
            down(step).wait_send()


def gather_over_tp(block, collective_id, weights=None, layer=0):
    count = lax.axis_size("tp")
    chips = count // 2
    rows, width = block.shape
    ring = 0 if weights is None else lax.axis_size("sp")
    operands = [block]
    in_specs = [pl.BlockSpec(memory_space=pltpu.VMEM)]
    out_shape = [jax.ShapeDtypeStruct((rows, width * count), block.dtype)]
    scratch = [pltpu.SemaphoreType.DMA((chips - 1,))] * 4
    scratch += [pltpu.SemaphoreType.DMA((2 * chips - 1,))] * 2
    if ring:
        operands.append(weights)
        in_specs.append(pl.BlockSpec(memory_space=pl.ANY))
        out_shape.append(
            jax.ShapeDtypeStruct((weights.shape[1] * ring, weights.shape[2]), weights.dtype)
        )
        scratch += [pltpu.SemaphoreType.DMA((ring // 2,))] * 4
        scratch += [pltpu.SemaphoreType.DMA]
    results = pl.pallas_call(
        functools.partial(gather_kernel, chips, ring, layer),
        out_shape=out_shape,
        in_specs=in_specs,
        out_specs=[pl.BlockSpec(memory_space=pltpu.VMEM)] * len(out_shape),
        scratch_shapes=scratch,
        compiler_params=pltpu.CompilerParams(
            collective_id=collective_id,
            has_side_effects=True,
            vmem_limit_bytes=(48 if ring else 16) * 2**20,
        ),
        cost_estimate=pl.CostEstimate(
            flops=COST_FLOPS, bytes_accessed=rows * width * count * 2, transcendentals=0
        ),
        name="gather_tp",
    )(*operands)
    return results if ring else results[0]


COST_FLOPS = 20 * 10**9


def sum_kernel(count, x_ref, out_ref, slots, sends, recvs):
    me = lax.axis_index("tp")
    barrier = pltpu.get_barrier_semaphore()
    for step in range(1, count):
        pl.semaphore_signal(
            barrier, inc=1, device_id={"tp": lax.rem(me + step, count)}, device_id_type=MESH
        )
    pl.semaphore_wait(barrier, count - 1)
    copies = [
        pltpu.make_async_remote_copy(
            src_ref=x_ref,
            dst_ref=slots.at[step - 1],
            send_sem=sends.at[step - 1],
            recv_sem=recvs.at[step - 1],
            device_id={"tp": lax.rem(me + step, count)},
            device_id_type=MESH,
        )
        for step in range(1, count)
    ]
    for copy in copies:
        copy.start()
    total = x_ref[...]
    for step in range(1, count):
        copies[step - 1].wait_recv()
        total = total + slots[step - 1]
    out_ref[...] = total
    for copy in copies:
        copy.wait_send()


def sum_over_tp(parts, collective_id):
    count = lax.axis_size("tp")
    flat = jnp.stack(parts).reshape(-1, 128)
    total = pl.pallas_call(
        functools.partial(sum_kernel, count),
        out_shape=jax.ShapeDtypeStruct(flat.shape, flat.dtype),
        in_specs=[pl.BlockSpec(memory_space=pltpu.VMEM)],
        out_specs=pl.BlockSpec(memory_space=pltpu.VMEM),
        scratch_shapes=[
            pltpu.VMEM((count - 1,) + flat.shape, flat.dtype),
            pltpu.SemaphoreType.DMA((count - 1,)),
            pltpu.SemaphoreType.DMA((count - 1,)),
        ],
        compiler_params=pltpu.CompilerParams(
            collective_id=collective_id, has_side_effects=True, vmem_limit_bytes=4 * 2**20
        ),
        cost_estimate=pl.CostEstimate(
            flops=COST_FLOPS // 8, bytes_accessed=flat.size * 8, transcendentals=0
        ),
        name="sum_tp",
    )(flat)
    return total.reshape(len(parts), -1)


def passed_along(value, axis, steps):
    count = lax.axis_size(axis)
    leading, last = (max(0, -steps), min(count, count - steps))
    return lax.ppermute(value, axis, [(source, source + steps) for source in range(leading, last)])


def shards(
    tokens, pre_gain, w_value, w_gate, conv_taps, conv_bias, norm_gain, norm_bias, w_out, post_gain
):
    layer_count = w_value.shape[0]
    tap_count = conv_taps.shape[1]
    channel_count = conv_taps.shape[2] * lax.axis_size("tp")
    model_width = tokens.shape[1] * lax.axis_size("tp")
    local_rows = tokens.shape[0]
    whole = []
    for layer_index in range(layer_count):
        per_layer = []
        for block in (w_gate, w_out):
            per_layer.append(lax.all_gather(block[layer_index], "sp", axis=0, tiled=True))
        whole.append(per_layer)
    stream = tokens
    for layer_index in range(layer_count):
        gate_block, out_block = whole[layer_index]
        if layer_index == 0:
            gathered, value_block = gather_over_tp(stream, 0, w_value, 0)
        else:
            gathered, value_block = gather_over_tp(stream, 4 * layer_index), next_value
        full_rows = gathered.astype(jnp.float32)
        scale_rows = lax.rsqrt(jnp.mean(full_rows * full_rows, axis=-1, keepdims=True) + 1e-06)
        normed = (full_rows * scale_rows * pre_gain[layer_index]).astype(jnp.bfloat16)
        value_proj = jnp.dot(normed, value_block, preferred_element_type=jnp.float32)
        gate_proj = jnp.dot(normed, gate_block, preferred_element_type=jnp.float32)
        glu_out = (value_proj * jax.nn.sigmoid(gate_proj)).astype(jnp.bfloat16)
        earlier = passed_along(glu_out[local_rows - (tap_count - 1) :], "sp", 1)
        padded = jnp.concatenate([earlier, glu_out], axis=0).astype(jnp.float32)
        filtered = jnp.zeros(glu_out.shape, jnp.float32) + conv_bias[layer_index]
        for tap_index in range(tap_count):
            filtered = (
                filtered
                + padded[tap_index : tap_index + local_rows] * conv_taps[layer_index, tap_index]
            )
        channel_sum, channel_square = sum_over_tp(
            (jnp.sum(filtered, axis=-1), jnp.sum(filtered * filtered, axis=-1)), 4 * layer_index + 1
        )
        centre = channel_sum / channel_count
        spread = jnp.maximum(channel_square / channel_count - centre * centre, 0.0)
        shaped = (filtered - centre[:, None]) * lax.rsqrt(spread + 1e-05)[:, None]
        mixed = jax.nn.silu(shaped * norm_gain[layer_index] + norm_bias[layer_index]).astype(
            jnp.bfloat16
        )
        if layer_index + 1 < layer_count:
            whole_mixed, next_value = gather_over_tp(
                mixed, 4 * layer_index + 2, w_value, layer_index + 1
            )
        else:
            whole_mixed = gather_over_tp(mixed, 4 * layer_index + 2)
        branch_low = jnp.dot(whole_mixed, out_block, preferred_element_type=jnp.float32).astype(
            jnp.bfloat16
        )
        branch = lax.optimization_barrier(branch_low).astype(jnp.float32)
        (total,) = sum_over_tp((jnp.sum(branch * branch, axis=-1),), 4 * layer_index + 3)
        rescale = lax.rsqrt(total / model_width + 1e-06)[:, None]
        stream = (stream.astype(jnp.float32) + branch * rescale * post_gain[layer_index]).astype(
            jnp.bfloat16
        )
    return stream


def solution(mesh):
    in_specs = (
        P("sp", "tp"),
        P(),
        P(None, "sp", "tp"),
        P(None, "sp", "tp"),
        P(None, None, "tp"),
        P(None, "tp"),
        P(None, "tp"),
        P(None, "tp"),
        P(None, "sp", "tp"),
        P(None, "tp"),
    )
    out_specs = P("sp", "tp")
    return jax.shard_map(shards, mesh=mesh, in_specs=in_specs, out_specs=out_specs, check_vma=False)
```
